32 devices in a mesh: fs: 4 (over y, x), tp: 8 (over z, core).
Axes of the slice: x: 2, y: 2, z: 4, core: 2. Of those that a mesh axis runs over, the one named last changes fastest.
Arguments:
- tokens: bfloat16 [4096, 2048], P(('fs', 'tp')), may hold values from -6 to 6
- norm_gain: float32 [2048], P('fs'), may hold values from 0.1 to 1.9
- gate_master: float32 [2048, 8192], P('fs', 'tp'), may hold values from -0.125 to 0.125
- up_master: float32 [2048, 8192], P('fs', 'tp'), may hold values from -0.125 to 0.125
- down_master: float32 [2048, 8192], P('fs', 'tp'), may hold values from -0.09375 to 0.09375
Outputs:
- mixed: bfloat16 [4096, 2048], P(('fs', 'tp'))
- gate_ready: bfloat16 [2048, 8192], P(None, 'tp')
- up_ready: bfloat16 [2048, 8192], P(None, 'tp')
- down_ready: bfloat16 [2048, 8192], P(None, 'tp')
The draws below stay inside these ranges and needn't reach their ends.
All inputs are finite; a program needn't handle non-finite values.
Results may differ from the reference program's by a relative error of at most 0.0095.
Values may be sent and summed in bfloat16 or wider, within the bound.
A program may use at most 64 MiB of HBM per device.

```python
import jax
import jax.numpy as jnp
from jax import lax

D = 2048
FF = 8192
TOKENS = 4096
N_TP = 8


def spiked(drawn, stream_key, source, target, blocks, factor):
    owner, partner = [(jnp.arange(drawn.shape[position]) // (drawn.shape[position] // blocks)).reshape([-1 if axis == position else 1 for axis in range(drawn.ndim)]) for position in (source, target)]
    chosen = jax.random.permutation(stream_key, blocks)[partner]
    strong = (owner == chosen) | (owner == (partner + blocks // 2) % blocks)
    return jnp.where(strong, factor * drawn, drawn)


def level_of(rng, shape, shards, low, high):
    loudness, own = 1.0, jax.random.fold_in(rng, 6)
    for dim, shards_of in shards:
        heights = jnp.exp(jax.random.uniform(jax.random.fold_in(own, dim), (shards_of,), jnp.float32, low / len(shards), high / len(shards)))
        loudness = loudness * jnp.repeat(heights, shape[dim] // shards_of).reshape([-1 if axis == dim else 1 for axis in range(len(shape))])
    return loudness


def centred(key, dims, spread, limit, cuts=(), dtype=jnp.bfloat16):
    drawn = spread * jax.random.normal(key, dims, jnp.float32)
    if cuts:
        drawn = drawn * level_of(key, dims, cuts, -0.22, 0.18)
    return jnp.clip(drawn, -limit, limit).astype(dtype)


def heavy_noise(key, dims, deviation, bound, split, heavy, held_as=jnp.bfloat16):
    drawn = deviation * jax.random.normal(key, dims, jnp.float32)
    if split:
        drawn = drawn * level_of(key, dims, split, -0.22, 0.18)
    return jnp.clip(spiked(drawn, jax.random.fold_in(key, 3), *heavy), -bound, bound).astype(held_as)


def setup_inputs(seed: int = 0) -> dict:
    key_of = jax.random.split(jax.random.key(seed), 6)
    tokens = centred(key_of[0], (TOKENS, D), 1.0, 6.0, ((0, 32),))
    norm_gain = jnp.clip(1.0 + 0.18 * jax.random.normal(key_of[1], (D,), jnp.float32), 0.1, 1.9)
    gate_master = centred(key_of[2], (D, FF), D ** -0.5, 0.125, ((0, 4), (1, 8)), jnp.float32)
    up_master = centred(key_of[3], (D, FF), D ** -0.5, 0.125, ((0, 4), (1, 8)), jnp.float32)
    down_master = heavy_noise(key_of[4], (D, FF), FF ** -0.5, 0.09375, ((0, 4), (1, 8)), (1, 0, 8, 2.0), jnp.float32)
    return {"tokens": tokens, "norm_gain": norm_gain, "gate_master": gate_master, "up_master": up_master, "down_master": down_master}


def reference(tokens, norm_gain, gate_master, up_master, down_master):
    gate_ready = (norm_gain[:, None] * gate_master).astype(jnp.bfloat16)
    up_ready = (norm_gain[:, None] * up_master).astype(jnp.bfloat16)
    down_ready = down_master.astype(jnp.bfloat16)
    tokens_wide = tokens.astype(jnp.float32)
    row_scale = lax.rsqrt(lax.optimization_barrier(jnp.mean(tokens_wide * tokens_wide, axis=1, keepdims=True)) + 1e-06)
    gate_proj = row_scale * jnp.dot(tokens, gate_ready, preferred_element_type=jnp.float32)
    up_proj = row_scale * jnp.dot(tokens, up_ready, preferred_element_type=jnp.float32)
    hidden = (jax.nn.silu(gate_proj) * up_proj).astype(jnp.bfloat16)
    block_width = FF // N_TP
    summed = jnp.zeros((tokens.shape[0], tokens.shape[1]), jnp.float32)
    for column_block in range(N_TP):
        lower = column_block * block_width
        partial_value = lax.dot_general(hidden[:, lower:lower + block_width], down_ready[:, lower:lower + block_width], (((1,), (1,)), ((), ())), preferred_element_type=jnp.float32)
        summed = summed + lax.optimization_barrier(partial_value.astype(jnp.bfloat16)).astype(jnp.float32)
    mixed = (tokens_wide + 0.5 * summed).astype(jnp.bfloat16)
    return (mixed, gate_ready, up_ready, down_ready)
```

```python
import functools

import jax
import jax.numpy as jnp
from jax import lax
from jax.experimental import pallas as pl
from jax.experimental.pallas import tpu as pltpu
from jax.sharding import PartitionSpec as P

MESH = pl.DeviceIdType.MESH
GATE, UP, DOWN = 0, 1, 2


def flip(index, bit):
    return index + bit - 2 * bit * ((index // bit) % 2)


def flip_all(index, mask, dims):
    for dim in range(dims):
        if mask >> dim & 1:
            index = flip(index, 1 << dim)
    return index


def span(bits):
    masks = [0]
    for bit in bits:
        masks += [mask | bit for mask in masks]
    return masks


def kernel(
    n_fs, n_z, dims, pieces,
    tok_in, gain, gate_master, up_master, down_master,
    mixed, gate, up, down,
    tok, scale, gate_acc, up_acc, hidden, pair_own, pair_send, pair_recv, z_send, z_recv,
    w_sent, w_got, t_sent, t_got, s_sent, s_got, p_sent, p_got, z_sent, z_got,
):
    fs, tp = lax.axis_index("fs"), lax.axis_index("tp")
    z, core = tp // 2, tp % 2
    sibling = z * 2 + 1 - core
    rows, cols = gate_master.shape
    part = rows // dims
    own_tok = tok_in.shape[0]
    half = n_z * own_tok
    total = 2 * half
    width = rows // pieces
    masters, ready = (gate_master, up_master, down_master), (gate, up, down)

    def z_peer(k):
        return ((z + k) % n_z) * 2 + core

    barrier = pltpu.get_barrier_semaphore()
    for dim in range(dims):
        pl.semaphore_signal(barrier, 1, device_id={"fs": flip(fs, 1 << dim)}, device_id_type=MESH)
    for k in range(1, n_z):
        pl.semaphore_signal(barrier, 1, device_id={"tp": z_peer(k)}, device_id_type=MESH)
    pl.semaphore_signal(barrier, 1, device_id={"tp": sibling}, device_id_type=MESH)
    pl.semaphore_wait(barrier, dims + n_z)

    def block(w, mask, p, count=1):
        start = flip_all(fs, mask, dims) * rows + p * part
        return ready[w].at[pl.ds(pl.multiple_of(start, part), part * count), :]

    def order(p):
        return [1 << ((p + s) % dims) for s in range(dims)]

    def weight_copy(w, p, stage, held):
        bit = order(p)[stage]
        mask = held | bit
        return pltpu.make_async_remote_copy(
            src_ref=block(w, held, p), dst_ref=block(w, held, p),
            send_sem=w_sent.at[w, p, mask], recv_sem=w_got.at[w, p, mask],
            device_id={"fs": flip(fs, bit)}, device_id_type=MESH,
        )

    arrivals = {}
    started, arrived = [], set()
    for p in range(dims):
        for stage in range(dims):
            for held in span(order(p)[:stage]):
                arrivals[p, held | order(p)[stage]] = (stage, held)

    def send(w, p, stage, held):
        copy = weight_copy(w, p, stage, held)
        copy.start()
        started.append(copy)

    def need(w, p, mask):
        if mask and (w, p, mask) not in arrived:
            arrived.add((w, p, mask))
            stage, held = arrivals[p, mask]
            pltpu.make_async_remote_copy(
                src_ref=block(w, mask, p), dst_ref=block(w, mask, p),
                send_sem=w_sent.at[w, p, mask], recv_sem=w_got.at[w, p, mask],
                device_id={"fs": flip(fs, order(p)[stage])}, device_id_type=MESH,
            ).wait_recv()

    def relays(ws):
        for stage in range(1, dims):
            for w in ws:
                for p in range(dims):
                    for mask in span(order(p)[:stage]):
                        if mask:
                            need(w, p, mask)
                            send(w, p, stage, mask)

    def prepare(w, p):
        mine = slice(p * part, (p + 1) * part)
        value = masters[w][mine, :]
        if w != DOWN:
            value = gain[mine, :] * value
        block(w, 0, p)[...] = value.astype(jnp.bfloat16)

    for w in (GATE, UP):
        for p in range(dims):
            prepare(w, p)
            send(w, p, 0, 0)

    def tok_rows(c, chip):
        start = (c * n_z + chip) * own_tok
        return tok.at[pl.ds(pl.multiple_of(start, own_tok), own_tok), :]

    def tok_z(k):
        return pltpu.make_async_remote_copy(
            src_ref=tok_in, dst_ref=tok_rows(core, z), send_sem=t_sent.at[k], recv_sem=t_got.at[k],
            device_id={"tp": z_peer(k)}, device_id_type=MESH,
        )

    def tok_sibling(k, src, slot):
        return pltpu.make_async_remote_copy(
            src_ref=src, dst_ref=slot, send_sem=s_sent.at[k], recv_sem=s_got.at[k],
            device_id={"tp": sibling}, device_id_type=MESH,
        )

    for k in range(1, n_z):
        copy = tok_z(k)
        copy.start()
        started.append(copy)
    copy = tok_sibling(0, tok_in, tok_rows(core, z))
    copy.start()
    started.append(copy)
    for w in (GATE, UP):
        for p in range(dims):
            for stage in range(1, dims):
                send(w, p, stage, 0)
    tok_rows(core, z)[...] = tok_in[...]
    for p in range(dims):
        prepare(DOWN, p)

    relays((GATE, UP))
    for p in range(dims):
        send(DOWN, p, 0, 0)
    for p in range(dims):
        for stage in range(1, dims):
            send(DOWN, p, stage, 0)

    for k in range(1, n_z):
        slot = tok_rows(core, (z + n_z - k) % n_z)
        pltpu.make_async_remote_copy(
            src_ref=slot, dst_ref=slot, send_sem=t_sent.at[k], recv_sem=t_got.at[k],
            device_id={"tp": z_peer(k)}, device_id_type=MESH,
        ).wait_recv()
        copy = tok_sibling(k, slot, slot)
        copy.start()
        started.append(copy)
    for k in range(n_z):
        slot = tok_rows(1 - core, (z + n_z - k) % n_z)
        tok_sibling(k, slot, slot).wait_recv()

    tile_m, tile_n = min(256, total), min(512, cols)
    tile_s = min(64, total)

    @pl.loop(0, total // tile_s)
    def _(i):
        at = pl.ds(pl.multiple_of(i * tile_s, tile_s), tile_s)
        wide = tok[at, :].astype(jnp.float32)
        scale[at, :] = lax.rsqrt(jnp.mean(wide * wide, axis=1, keepdims=True) + 1e-06)

    for mask in range(n_fs):
        for w in (GATE, UP):
            for p in range(dims):
                need(w, p, mask)
        owner = flip_all(fs, mask, dims)
        deep = pl.ds(pl.multiple_of(owner * rows, rows), rows)
        first, last = mask == 0, mask == n_fs - 1

        @pl.loop(0, (total // tile_m) * (cols // tile_n))
        def _(i):
            across = cols // tile_n
            at = pl.ds(pl.multiple_of((i // across) * tile_m, tile_m), tile_m)
            to = pl.ds(pl.multiple_of((i % across) * tile_n, tile_n), tile_n)
            x = tok[at, deep]
            g = jnp.dot(x, gate[deep, to], preferred_element_type=jnp.float32)
            u = jnp.dot(x, up[deep, to], preferred_element_type=jnp.float32)
            if not first:
                g = g + gate_acc[at, to]
                u = u + up_acc[at, to]
            if last:
                g = scale[at, :] * g
                u = scale[at, :] * u
                hidden[at, to] = (g / (1.0 + jnp.exp(-g)) * u).astype(jnp.bfloat16)
            else:
                gate_acc[at, to] = g
                up_acc[at, to] = u

    def product(parity, start, out, add=None):
        tile = min(256, half)

        @pl.loop(0, half // tile)
        def _(i):
            at = pl.ds(pl.multiple_of(i * tile, tile), tile)
            src = pl.ds(pl.multiple_of(parity * half + i * tile, tile), tile)
            value = lax.dot_general(
                hidden[src, :], down[pl.ds(pl.multiple_of(start, width), width), :],
                (((1,), (1,)), ((), ())), preferred_element_type=jnp.float32,
            )
            out[at, :] = value.astype(out.dtype)

    def pair_copy(n):
        return pltpu.make_async_remote_copy(
            src_ref=pair_send.at[n], dst_ref=pair_recv.at[n],
            send_sem=p_sent.at[n], recv_sem=p_got.at[n],
            device_id={"tp": sibling}, device_id_type=MESH,
        )

    def z_copy(n, k):
        slot = pl.ds(pl.multiple_of(((z + k) % n_z) * own_tok, own_tok), own_tok)
        return pltpu.make_async_remote_copy(
            src_ref=z_send.at[n, slot, :], dst_ref=z_recv.at[n, k - 1],
            send_sem=z_sent.at[n, k], recv_sem=z_got.at[n, k],
            device_id={"tp": z_peer(k)}, device_id_type=MESH,
        )

    chunks = []
    late = sorted(
        ((mask, q) for mask in range(n_fs) for q in range(pieces)),
        key=lambda c: (
            0 if c[0] == 0 else 1 + max(
                2 * arrivals[p, c[0]][0] + bin(c[0]).count("1") * 4
                for p in ((c[1],) if pieces == dims else range(dims))
            ), c[0], c[1],
        ),
    )

    def finish(n):
        pair_copy(n).wait_recv()
        z_send[n] = (pair_own[n % 2] + pair_recv[n].astype(jnp.float32)).astype(jnp.bfloat16)
        for k in range(n_z - 1, 0, -1):
            copy = z_copy(n, k)
            copy.start()
            started.append(copy)

    relayed = False
    for n, (mask, q) in enumerate(late):
        if mask and not relayed:
            relayed = True
            relays((DOWN,))
        for p in (q,) if pieces == dims else range(dims):
            need(DOWN, p, mask)
        start = flip_all(fs, mask, dims) * rows + q * width
        product(1 - core, start, pair_send.at[n])
        copy = pair_copy(n)
        copy.start()
        started.append(copy)
        product(core, start, pair_own.at[n % 2])
        chunks.append(start)
        finish(n)

    for n, start in enumerate(chunks):
        for k in range(1, n_z):
            z_copy(n, k).wait_recv()
        mine = pl.ds(pl.multiple_of(z * own_tok, own_tok), own_tok)
        branch = z_send[n, mine, :].astype(jnp.float32)
        for k in range(1, n_z):
            branch = branch + z_recv[n, k - 1].astype(jnp.float32)
        to = pl.ds(pl.multiple_of(start, width), width)
        mixed[:, to] = (tok_in[:, to].astype(jnp.float32) + 0.5 * branch).astype(jnp.bfloat16)

    for copy in started:
        copy.wait_send()


def body(n_fs, n_tp, tokens, norm_gain, gate_master, up_master, down_master):
    own_tok, depth = tokens.shape
    rows, cols = gate_master.shape
    dims = n_fs.bit_length() - 1
    n_z = n_tp // 2
    half, total = n_z * own_tok, n_tp * own_tok
    part = rows // dims
    pieces = dims if part % 128 == 0 else 1
    width, count = rows // pieces, n_fs * pieces
    bf16, f32 = jnp.bfloat16, jnp.float32
    dma = pltpu.SemaphoreType.DMA
    vmem = pl.BlockSpec(memory_space=pltpu.VMEM)
    return pl.pallas_call(
        functools.partial(kernel, n_fs, n_z, dims, pieces),
        out_shape=(jax.ShapeDtypeStruct((own_tok, depth), bf16),)
        + tuple(pltpu.VMEM((n_fs * rows, cols), bf16) for _ in range(3)),
        in_specs=[vmem] * 5,
        out_specs=(vmem,) * 4,
        scratch_shapes=[
            pltpu.VMEM((total, depth), bf16),
            pltpu.VMEM((total, 1), f32),
            pltpu.VMEM((total, cols), f32),
            pltpu.VMEM((total, cols), f32),
            pltpu.VMEM((total, cols), bf16),
            pltpu.VMEM((2, half, width), f32),
            pltpu.VMEM((count, half, width), bf16),
            pltpu.VMEM((count, half, width), bf16),
            pltpu.VMEM((count, half, width), bf16),
            pltpu.VMEM((count, n_z - 1, own_tok, width), bf16),
            dma((3, dims, n_fs)), dma((3, dims, n_fs)),
            dma((n_z,)), dma((n_z,)),
            dma((n_z,)), dma((n_z,)),
            dma((count,)), dma((count,)),
            dma((count, n_z)), dma((count, n_z)),
        ],
        compiler_params=pltpu.CompilerParams(
            collective_id=0, has_side_effects=True, vmem_limit_bytes=40 * 1024 * 1024
        ),
    )(tokens, norm_gain[:, None], gate_master, up_master, down_master)


def solution(mesh):
    in_specs = (P(("fs", "tp"), None), P("fs"), P("fs", "tp"), P("fs", "tp"), P("fs", "tp"))
    out_specs = (P(("fs", "tp"), None), P(None, "tp"), P(None, "tp"), P(None, "tp"))
    step = functools.partial(body, mesh.shape["fs"], mesh.shape["tp"])
    return jax.shard_map(step, mesh=mesh, in_specs=in_specs, out_specs=out_specs, check_vma=False)
```

```python
import functools

import jax
import jax.numpy as jnp
from jax import lax
from jax.experimental import pallas as pl
from jax.experimental.pallas import tpu as pltpu
from jax.sharding import PartitionSpec as P

MESH = pl.DeviceIdType.MESH
GATE, UP, DOWN = 0, 1, 2


def flip(index, bit):
    return index + bit - 2 * bit * ((index // bit) % 2)


def flip_all(index, mask, dims):
    for dim in range(dims):
        if mask >> dim & 1:
            index = flip(index, 1 << dim)
    return index


def span(bits):
    masks = [0]
    for bit in bits:
        masks += [mask | bit for mask in masks]
    return masks


def kernel(
    n_fs, n_z, dims, halves, pieces,
    tok_hbm, gain_hbm, gate_hbm, up_hbm, down_hbm,
    mixed, gate, up, down,
    tok_in, gain_row, gain, masters, tok, scale, gate_acc, up_acc, hidden, pair_own, pair_send, pair_recv, z_send, z_recv, ahead,
    w_sent, w_got, t_sent, t_got, s_sent, s_got, p_sent, p_got, z_sent, z_got, a_sent, a_got, loaded,
):
    fs, tp = lax.axis_index("fs"), lax.axis_index("tp")
    z, core = tp // 2, tp % 2
    sibling = z * 2 + 1 - core
    rows, cols = gate_hbm.shape
    part = rows // dims
    own_tok = tok_in.shape[0]
    half = n_z * own_tok
    total = 2 * half
    width = rows // pieces
    ready = (gate, up, down)

    loads = {}
    reads = [("gain", gain_hbm, gain_row)]
    for p in range(dims):
        mine = pl.ds(p * part, part)
        reads.append(((GATE, p), gate_hbm.at[mine, :], masters.at[GATE, mine, :]))
    for p in range(dims):
        mine = pl.ds(p * part, part)
        reads.append(((UP, p), up_hbm.at[mine, :], masters.at[UP, mine, :]))
    reads.append(("tok", tok_hbm, tok_in))
    reads.append(((DOWN, 0), down_hbm, masters.at[DOWN]))
    for n, (name, src, dst) in enumerate(reads):
        loads[name] = pltpu.make_async_copy(src, dst, loaded.at[n])
        loads[name].start()

    def z_peer(k):
        return ((z + k) % n_z) * 2 + core

    barrier = pltpu.get_barrier_semaphore()
    for dim in range(dims):
        pl.semaphore_signal(barrier, 1, device_id={"fs": flip(fs, 1 << dim)}, device_id_type=MESH)
    for k in range(1, n_z):
        pl.semaphore_signal(barrier, 1, device_id={"tp": z_peer(k)}, device_id_type=MESH)
    pl.semaphore_signal(barrier, 1, device_id={"tp": sibling}, device_id_type=MESH)
    pl.semaphore_wait(barrier, dims + n_z)

    loads["gain"].wait()
    for n in range(rows // 128):
        line = gain_row[:, n * 128:(n + 1) * 128]
        gain[n * 128:(n + 1) * 128, :] = jnp.transpose(jnp.broadcast_to(line, (128, 128)))

    cuts = (1, 1, halves)

    def block(w, mask, p, h):
        tall = part // cuts[w]
        start = flip_all(fs, mask, dims) * rows + p * part + h * tall
        return ready[w].at[pl.ds(pl.multiple_of(start, tall), tall), :]

    def order(p):
        return [1 << ((p + s) % dims) for s in range(dims)]

    arrivals = {
        (p, held | order(p)[stage]): stage
        for p in range(dims) for stage in range(dims) for held in span(order(p)[:stage])
    }
    started, arrived = [], set()

    def weight_copy(w, p, h, held, mask, stage):
        return pltpu.make_async_remote_copy(
            src_ref=block(w, held, p, h), dst_ref=block(w, held, p, h),
            send_sem=w_sent.at[w, p, h, mask], recv_sem=w_got.at[w, p, h, mask],
            device_id={"fs": flip(fs, order(p)[stage])}, device_id_type=MESH,
        )

    def launch(copy):
        copy.start()
        started.append(copy)

    def send(w, p, h, stage, held):
        launch(weight_copy(w, p, h, held, held | order(p)[stage], stage))

    def need(w, p, h, mask):
        if mask and (w, p, h, mask) not in arrived:
            arrived.add((w, p, h, mask))
            stage = arrivals[p, mask]
            weight_copy(w, p, h, mask, mask, stage).wait_recv()
            for later in range(stage + 1, dims):
                send(w, p, h, later, mask)

    def relays(ws):
        for stage in range(dims - 1):
            for w in ws:
                for p in range(dims):
                    for held in span(order(p)[:stage]):
                        for h in range(cuts[w]):
                            need(w, p, h, held | order(p)[stage])

    def prepare(w, p):
        mine = slice(p * part, (p + 1) * part)
        if (w, p) in loads:
            loads[w, p].wait()
        value = masters[w, mine, :]
        if w != DOWN:
            value = gain[mine, 0:1] * value
        ready[w][pl.ds(pl.multiple_of(fs * rows + p * part, part), part), :] = value.astype(jnp.bfloat16)

    for p in range(dims):
        prepare(GATE, p)
        send(GATE, p, 0, 0, 0)
    for p in range(dims):
        prepare(UP, p)
        send(UP, p, 0, 0, 0)

    def tok_rows(c, chip):
        start = (c * n_z + chip) * own_tok
        return tok.at[pl.ds(pl.multiple_of(start, own_tok), own_tok), :]

    def tok_z(k):
        return pltpu.make_async_remote_copy(
            src_ref=tok_in, dst_ref=tok_rows(core, z), send_sem=t_sent.at[k], recv_sem=t_got.at[k],
            device_id={"tp": z_peer(k)}, device_id_type=MESH,
        )

    def tok_sibling(k, src, slot):
        return pltpu.make_async_remote_copy(
            src_ref=src, dst_ref=slot, send_sem=s_sent.at[k], recv_sem=s_got.at[k],
            device_id={"tp": sibling}, device_id_type=MESH,
        )

    loads["tok"].wait()
    for k in range(1, n_z):
        launch(tok_z(k))
    launch(tok_sibling(0, tok_in, tok_rows(core, z)))
    for w in (GATE, UP):
        for p in range(dims):
            for stage in range(1, dims):
                send(w, p, 0, stage, 0)
    tok_rows(core, z)[...] = tok_in[...]
    for p in range(dims):
        prepare(DOWN, p)

    relays((GATE, UP))
    for stage in range(dims):
        for h in range(halves):
            for p in range(dims):
                send(DOWN, p, h, stage, 0)

    for k in range(1, n_z):
        slot = tok_rows(core, (z + n_z - k) % n_z)
        pltpu.make_async_remote_copy(
            src_ref=slot, dst_ref=slot, send_sem=t_sent.at[k], recv_sem=t_got.at[k],
            device_id={"tp": z_peer(k)}, device_id_type=MESH,
        ).wait_recv()
        launch(tok_sibling(k, slot, slot))
    for k in range(n_z):
        slot = tok_rows(1 - core, (z + n_z - k) % n_z)
        tok_sibling(k, slot, slot).wait_recv()

    tile_m, tile_n = min(256, total), min(512, cols)
    tile_s = min(64, total)

    @pl.loop(0, total // tile_s)
    def _(i):
        at = pl.ds(pl.multiple_of(i * tile_s, tile_s), tile_s)
        wide = tok[at, :].astype(jnp.float32)
        scale[at, :] = lax.rsqrt(jnp.mean(wide * wide, axis=1, keepdims=True) + 1e-06)

    for mask in range(n_fs):
        for w in (GATE, UP):
            for p in range(dims):
                need(w, p, 0, mask)
        owner = flip_all(fs, mask, dims)
        deep = pl.ds(pl.multiple_of(owner * rows, rows), rows)
        first, last = mask == 0, mask == n_fs - 1

        @pl.loop(0, (total // tile_m) * (cols // tile_n))
        def _(i):
            across = cols // tile_n
            at = pl.ds(pl.multiple_of((i // across) * tile_m, tile_m), tile_m)
            to = pl.ds(pl.multiple_of((i % across) * tile_n, tile_n), tile_n)
            x = tok[at, deep]
            g = jnp.dot(x, gate[deep, to], preferred_element_type=jnp.float32)
            u = jnp.dot(x, up[deep, to], preferred_element_type=jnp.float32)
            if not first:
                g = g + gate_acc[at, to]
                u = u + up_acc[at, to]
            if last:
                g = scale[at, :] * g
                u = scale[at, :] * u
                hidden[at, to] = (g / (1.0 + jnp.exp(-g)) * u).astype(jnp.bfloat16)
            else:
                gate_acc[at, to] = g
                up_acc[at, to] = u

    def product(parity, start, out, add=None):
        tile = min(256, half)

        @pl.loop(0, half // tile)
        def _(i):
            at = pl.ds(pl.multiple_of(i * tile, tile), tile)
            src = pl.ds(pl.multiple_of(parity * half + i * tile, tile), tile)
            value = lax.dot_general(
                hidden[src, :], down[pl.ds(pl.multiple_of(start, width), width), :],
                (((1,), (1,)), ((), ())), preferred_element_type=jnp.float32,
            )
            out[at, :] = value.astype(out.dtype)

    def pair_copy(n):
        return pltpu.make_async_remote_copy(
            src_ref=pair_send.at[n], dst_ref=pair_recv.at[n],
            send_sem=p_sent.at[n], recv_sem=p_got.at[n],
            device_id={"tp": sibling}, device_id_type=MESH,
        )

    def z_copy(n, k):
        slot = pl.ds(pl.multiple_of(((z + k) % n_z) * own_tok, own_tok), own_tok)
        return pltpu.make_async_remote_copy(
            src_ref=z_send.at[n, slot, :], dst_ref=z_recv.at[n, k - 1],
            send_sem=z_sent.at[n, k], recv_sem=z_got.at[n, k],
            device_id={"tp": z_peer(k)}, device_id_type=MESH,
        )

    merge = n_z > 2

    def goes_ahead(k):
        return ((z == 0) & (k == n_z - 1)) | ((z == n_z - 1) & (k == 1))

    def ahead_copy(n, k):
        slot = pl.ds(pl.multiple_of(((z + k) % n_z) * own_tok, own_tok), own_tok)
        return pltpu.make_async_remote_copy(
            src_ref=z_send.at[n, slot, :], dst_ref=ahead.at[n], send_sem=a_sent.at[n], recv_sem=a_got.at[n],
            device_id={"tp": (z + 1 if k == n_z - 1 else z - 1) * 2 + core}, device_id_type=MESH,
        )

    def joins(k):
        return ((z == 1) & (k == n_z - 2)) | ((z == n_z - 2) & (k == 2))

    def finish(n):
        pair_copy(n).wait_recv()
        z_send[n] = (pair_own[n % 2] + pair_recv[n].astype(jnp.float32)).astype(jnp.bfloat16)
        if merge:
            for k in (1, n_z - 1):
                @pl.when(goes_ahead(k))
                def _():
                    ahead_copy(n, k).start()
        for k in range(n_z - 1, 0, -1):
            if merge:
                @pl.when(jnp.logical_not(goes_ahead(k) | joins(k)))
                def _():
                    z_copy(n, k).start()
            else:
                z_copy(n, k).start()

    def join(n):
        if merge:
            for k in sorted({2, n_z - 2}):
                @pl.when(joins(k))
                def _():
                    slot = pl.ds(pl.multiple_of(((z + k) % n_z) * own_tok, own_tok), own_tok)
                    pltpu.make_async_remote_copy(
                        src_ref=ahead.at[n], dst_ref=ahead.at[n], send_sem=a_sent.at[n], recv_sem=a_got.at[n],
                        device_id={"tp": sibling}, device_id_type=MESH,
                    ).wait_recv()
                    both = z_send[n, slot, :].astype(jnp.float32) + ahead[n].astype(jnp.float32)
                    z_send[n, slot, :] = both.astype(jnp.bfloat16)
                    z_copy(n, k).start()

    def when_block(mask, p, h):
        return (0,) if mask == 0 else (1, bin(mask).count("1") > 1, arrivals[p, mask], h, p)

    blocks = [(mask, p, h) for mask in range(n_fs) for p in range(dims) for h in range(halves)]
    if pieces == 1:
        chunks = [[(mask, p, h) for p in range(dims) for h in range(halves)] for mask in range(n_fs)]
    else:
        chunks = [[b] for b in sorted(blocks, key=lambda b: when_block(*b))]
    starts = []
    for n, chunk in enumerate(chunks):
        for mask, p, h in chunk:
            need(DOWN, p, h, mask)
        mask, p, h = chunk[0]
        start = flip_all(fs, mask, dims) * rows + p * part + h * width
        starts.append(start)
        product(1 - core, start, pair_send.at[n])
        launch(pair_copy(n))
        if n:
            finish(n - 1)
        if n > 1:
            join(n - 2)
        product(core, start, pair_own.at[n % 2])
    finish(len(chunks) - 1)
    for n in range(max(0, len(chunks) - 2), len(chunks)):
        join(n)

    for n, start in enumerate(starts):
        mine = pl.ds(pl.multiple_of(z * own_tok, own_tok), own_tok)
        to = pl.ds(pl.multiple_of(start, width), width)
        branch = z_send[n, mine, :].astype(jnp.float32)
        for k in range(1, n_z):
            if merge and k in (1, n_z - 1):
                far = ((z == n_z - 1) & (k == n_z - 1)) | ((z == 0) & (k == 1))

                @pl.when(jnp.logical_not(far))
                def _():
                    z_copy(n, k).wait_recv()

                @pl.when(far)
                def _():
                    z_recv[n, k - 1] = jnp.zeros((own_tok, width), jnp.bfloat16)
            else:
                z_copy(n, k).wait_recv()
            branch = branch + z_recv[n, k - 1].astype(jnp.float32)
        mixed[:, to] = (tok_in[:, to].astype(jnp.float32) + 0.5 * branch).astype(jnp.bfloat16)

    for n in range(len(chunks)):
        for k in range(1, n_z):
            if merge and k in (1, n_z - 1):
                @pl.when(goes_ahead(k))
                def _():
                    ahead_copy(n, k).wait_send()

                @pl.when(jnp.logical_not(goes_ahead(k)))
                def _():
                    z_copy(n, k).wait_send()
            else:
                z_copy(n, k).wait_send()
    for copy in started:
        copy.wait_send()


def store(*refs):
    count = len(refs) // 2
    done = refs[-1]
    copies = []
    for n in range(count):
        tall = refs[n].shape[0] // 2
        for h in range(2):
            at = pl.ds(h * tall, tall)
            copies.append(pltpu.make_async_copy(refs[n].at[at, :], refs[count + n].at[at, :], done.at[n, h]))
            copies[-1].start()
    for copy in copies:
        copy.wait()


def body(n_fs, n_tp, tokens, norm_gain, gate_master, up_master, down_master):
    own_tok, depth = tokens.shape
    rows, cols = gate_master.shape
    dims = n_fs.bit_length() - 1
    n_z = n_tp // 2
    half, total = n_z * own_tok, n_tp * own_tok
    part = rows // dims
    halves = part // 128 if part % 128 == 0 else 1
    pieces = dims * halves if part % 128 == 0 else 1
    width, count = rows // pieces, n_fs * pieces
    bf16, f32 = jnp.bfloat16, jnp.float32
    dma = pltpu.SemaphoreType.DMA
    vmem = pl.BlockSpec(memory_space=pltpu.VMEM)
    hbm = pl.BlockSpec(memory_space=pltpu.HBM)
    operands = (tokens, norm_gain[None, :], gate_master, up_master, down_master)
    results = pl.pallas_call(
        functools.partial(kernel, n_fs, n_z, dims, halves, pieces),
        out_shape=(pltpu.VMEM((own_tok, depth), bf16),)
        + tuple(pltpu.VMEM((n_fs * rows, cols), bf16) for _ in range(3)),
        in_specs=[hbm] * 5,
        out_specs=(vmem,) * 4,
        scratch_shapes=[
            pltpu.VMEM((own_tok, depth), bf16),
            pltpu.VMEM((1, rows), f32),
            pltpu.VMEM((rows, 128), f32),
            pltpu.VMEM((3, rows, cols), f32),
            pltpu.VMEM((total, depth), bf16),
            pltpu.VMEM((total, 1), f32),
            pltpu.VMEM((total, cols), f32),
            pltpu.VMEM((total, cols), f32),
            pltpu.VMEM((total, cols), bf16),
            pltpu.VMEM((2, half, width), f32),
            pltpu.VMEM((count, half, width), bf16),
            pltpu.VMEM((count, half, width), bf16),
            pltpu.VMEM((count, half, width), bf16),
            pltpu.VMEM((count, n_z - 1, own_tok, width), bf16),
            pltpu.VMEM((count, own_tok, width), bf16),
            dma((3, dims, halves, n_fs)), dma((3, dims, halves, n_fs)),
            dma((n_z,)), dma((n_z,)),
            dma((n_z,)), dma((n_z,)),
            dma((count,)), dma((count,)),
            dma((count, n_z)), dma((count, n_z)),
            dma((count,)), dma((count,)),
            dma((2 * dims + 3,)),
        ],
        compiler_params=pltpu.CompilerParams(
            collective_id=0, has_side_effects=True, vmem_limit_bytes=40 * 1024 * 1024
        ),
    )(*(pltpu.with_memory_space_constraint(value, pltpu.HBM) for value in operands))
    return pl.pallas_call(
        store,
        out_shape=tuple(jax.ShapeDtypeStruct(result.shape, result.dtype) for result in results),
        in_specs=[vmem] * 4,
        out_specs=(hbm,) * 4,
        scratch_shapes=[dma((4, 2))],
        compiler_params=pltpu.CompilerParams(vmem_limit_bytes=1024 * 1024),
    )(*(pltpu.with_memory_space_constraint(result, pltpu.VMEM) for result in results))


def solution(mesh):
    in_specs = (P(("fs", "tp"), None), P("fs"), P("fs", "tp"), P("fs", "tp"), P("fs", "tp"))
    out_specs = (P(("fs", "tp"), None), P(None, "tp"), P(None, "tp"), P(None, "tp"))
    step = functools.partial(body, mesh.shape["fs"], mesh.shape["tp"])
    return jax.shard_map(step, mesh=mesh, in_specs=in_specs, out_specs=out_specs, check_vma=False)
```
